32 devices in a mesh: sp: 8 (over z, y), tp: 4 (over x, core).
Axes of the slice: x: 2, y: 2, z: 4, core: 2. Of those that a mesh axis runs over, the one named last changes fastest.
Arguments:
- resid: bfloat16 [6144, 2048], P(('sp', 'tp')), may hold values from -6 to 6
- query_small: bfloat16 [6144, 768], P('sp', 'tp'), may hold values from -480 to 480
- query_large: bfloat16 [6144, 1280], P('sp', 'tp'), may hold values from -480 to 480
- kv_latent: bfloat16 [6144, 256], P('sp'), may hold values from -6 to 6
- rope_key: bfloat16 [6144, 32], P('sp'), may hold values from -6 to 6
- kv_gain: bfloat16 [256], replicated, may hold values from 0.099609375 to 1.8984375
- up_key_small: bfloat16 [256, 512], P(None, 'tp'), may hold values from -0.375 to 0.375
- up_value_small: bfloat16 [256, 512], P(None, 'tp'), may hold values from -0.375 to 0.375
- up_key_large: bfloat16 [256, 1024], P(None, 'tp'), may hold values from -0.375 to 0.375
- up_value_large: bfloat16 [256, 1024], P(None, 'tp'), may hold values from -0.375 to 0.375
- out_weight: bfloat16 [1536, 2048], replicated, may hold values from -0.359375 to 0.359375
- mix_gain: bfloat16 [2048], replicated, may hold values from 0.099609375 to 1.8984375
- gate_weight: bfloat16 [2048, 5632], P('sp', 'tp'), may hold values from -0.125 to 0.125
- up_weight: bfloat16 [2048, 5632], P('sp', 'tp'), may hold values from -0.125 to 0.125
- down_weight: bfloat16 [2048, 5632], P('sp', 'tp'), may hold values from -0.078125 to 0.078125
Outputs:
- layer_output: bfloat16 [6144, 2048], P(('sp', 'tp'))
The draws below stay inside these ranges and needn't reach their ends.
All inputs are finite; a program needn't handle non-finite values.
Results may differ from the reference program's by a relative error of at most 0.014.
The reference program's roundings to bfloat16 on the way count: a program that leaves them out, or rounds other values in their place, can miss the bound.
Values may be sent and summed in bfloat16 or wider, within the bound.
A program may use at most 128 MiB of HBM per device.

```python
import math
import jax
import jax.numpy as jnp
from jax import lax

D = 2048
HEADS_SMALL = 8
HEADS_LARGE = 8
NOPE_SMALL = 64
NOPE_LARGE = 128
VALUE_SMALL = 64
VALUE_LARGE = 128
ROTARY = 32
LATENT = 256
FF = 5632
TOK_DEV = 768
SEQ = 6144
N_TP = 4


def drawn_query(key, columns):
    base = 2.0 * jax.random.truncated_normal(key, -6.0, 6.0, (SEQ, columns), jnp.float32)
    return base


def draw_query_small(key, part):
    return drawn_query(jax.random.fold_in(key, 11), HEADS_SMALL * (NOPE_SMALL + ROTARY)).astype(jnp.bfloat16)


def draw_query_large(key, part):
    return drawn_query(jax.random.fold_in(key, 13), HEADS_LARGE * (NOPE_LARGE + ROTARY)).astype(jnp.bfloat16)


def steps_of(key, shape, split, low, high):
    loudness = 1.0
    for dim, shards_of in split:
        steps = jax.random.uniform(jax.random.fold_in(jax.random.fold_in(key, 6), dim), (shards_of,), jnp.float32, low / len(split), high / len(split))
        loudness = loudness * jnp.repeat(jnp.exp(steps), shape[dim] // shards_of).reshape((-1,) + (1,) * (len(shape) - 1 - dim))
    return loudness


def normal_values(own_key, extent, scale, bound, shards=(), held_as=jnp.bfloat16):
    factor_of = steps_of(own_key, extent, shards, -0.22, 0.18) if shards else 1.0
    drawn = jax.random.normal(own_key, extent, jnp.float32) * scale * factor_of
    return jnp.minimum(jnp.maximum(drawn, -bound), bound).astype(held_as)


def setup_inputs(seed: int = 0) -> dict:
    arg_keys = jax.random.split(jax.random.key(seed), 16)
    return {
        "resid": normal_values(arg_keys[0], (SEQ, D), 1.0, 6.0, ((0, 32),)),
        "query_small": draw_query_small(jax.random.fold_in(arg_keys[15], 71), 0),
        "query_large": draw_query_large(jax.random.fold_in(arg_keys[15], 71), 0),
        "kv_latent": normal_values(arg_keys[3], (SEQ, LATENT), 1.0, 6.0, ((0, 8),)),
        "rope_key": normal_values(arg_keys[4], (SEQ, ROTARY), 1.0, 6.0, ((0, 8),)),
        "kv_gain": jnp.clip(1.0 + 0.18 * jax.random.normal(arg_keys[5], (LATENT,), jnp.float32), 0.099609375, 1.8984375).astype(jnp.bfloat16),
        "up_key_small": normal_values(arg_keys[6], (LATENT, HEADS_SMALL * NOPE_SMALL), LATENT ** -0.5, 0.375, ((1, 4),)),
        "up_value_small": normal_values(arg_keys[7], (LATENT, HEADS_SMALL * VALUE_SMALL), LATENT ** -0.5, 0.375, ((1, 4),)),
        "up_key_large": normal_values(arg_keys[8], (LATENT, HEADS_LARGE * NOPE_LARGE), LATENT ** -0.5, 0.375, ((1, 4),)),
        "up_value_large": normal_values(arg_keys[9], (LATENT, HEADS_LARGE * VALUE_LARGE), LATENT ** -0.5, 0.375, ((1, 4),)),
        "out_weight": normal_values(arg_keys[10], (HEADS_SMALL * VALUE_SMALL + HEADS_LARGE * VALUE_LARGE, D), 0.06, 0.359375),
        "mix_gain": jnp.clip(1.0 + 0.18 * jax.random.normal(arg_keys[11], (D,), jnp.float32), 0.099609375, 1.8984375).astype(jnp.bfloat16),
        "gate_weight": normal_values(arg_keys[12], (D, FF), D ** -0.5, 0.125, ((0, 8), (1, 4))),
        "up_weight": normal_values(arg_keys[13], (D, FF), D ** -0.5, 0.125, ((0, 8), (1, 4))),
        "down_weight": normal_values(arg_keys[14], (D, FF), FF ** -0.5, 0.078125, ((0, 8), (1, 4))),
    }


THETA = 10000.0
EPSILON = 1e-06
FLOOR = -1e+30

def angles(positions, width):
    inverse = THETA ** (-jnp.arange(0, width, 2).astype(jnp.float32) / width)
    phase = positions.astype(jnp.float32)[:, None] * inverse[None, :]
    return (jnp.cos(phase), jnp.sin(phase))

def rotate(values, angle_cos, angle_sin):
    half = values.shape[-1] // 2
    first = values[..., :half].astype(jnp.float32)
    second = values[..., half:].astype(jnp.float32)
    turned = jnp.concatenate([first * angle_cos - second * angle_sin, second * angle_cos + first * angle_sin], axis=-1)
    return turned.astype(jnp.bfloat16)

def norm_rows(values, gain):
    wide = values.astype(jnp.float32)
    scaled = wide * lax.rsqrt(lax.optimization_barrier(jnp.mean(wide * wide, axis=-1, keepdims=True)) + EPSILON)
    return (scaled * gain.astype(jnp.float32)).astype(jnp.bfloat16)

def attend(query, key_nope, shared_key, values, nope):
    length = query.shape[0]
    heads = query.shape[1]
    scale = 1.0 / math.sqrt(nope + shared_key.shape[1])
    count = length // TOK_DEV
    key_wide = key_nope.astype(jnp.float32)
    shared_wide = shared_key.astype(jnp.float32)
    value_wide = values.astype(jnp.float32)

    def one_block(index):
        start = index * TOK_DEV
        block = lax.dynamic_slice_in_dim(query, start, TOK_DEV, 0).astype(jnp.float32)
        scores = jnp.einsum('qhd,khd->hqk', block[..., :nope], key_wide)
        scores = scores + jnp.einsum('qhd,kd->hqk', block[..., nope:], shared_wide)
        scores = scores * scale
        query_pos = start + jnp.arange(TOK_DEV).astype(jnp.int32)
        key_pos = jnp.arange(length).astype(jnp.int32)
        allowed = key_pos[None, :] <= query_pos[:, None]
        scores = jnp.where(allowed[None], scores, FLOOR)
        maximum = lax.optimization_barrier(jnp.max(scores, axis=-1, keepdims=True))
        weights = jnp.where(allowed[None], jnp.exp(scores - maximum), 0.0)
        total = lax.optimization_barrier(jnp.sum(weights, axis=-1))
        rounded = lax.optimization_barrier(weights.astype(jnp.bfloat16)).astype(jnp.float32)
        summed = jnp.einsum('hqk,khd->qhd', rounded, value_wide)
        return (summed / jnp.transpose(total)[:, :, None]).astype(jnp.bfloat16)
    out = lax.map(one_block, jnp.arange(count).astype(jnp.int32))
    return out.reshape(length, -1)

def reference(resid, query_small, query_large, kv_latent, rope_key, kv_gain, up_key_small, up_value_small, up_key_large, up_value_large, out_weight, mix_gain, gate_weight, up_weight, down_weight):
    length = kv_latent.shape[0]
    positions = jnp.arange(length).astype(jnp.int32)
    angle_cos, angle_sin = angles(positions, ROTARY)
    latent_normed = norm_rows(kv_latent, kv_gain)
    rotated_key = rotate(rope_key, angle_cos, angle_sin)

    def group(query, up_key, up_value, heads, nope, width):
        shaped = query.reshape(length, heads, nope + ROTARY)
        turned = rotate(shaped[..., nope:], angle_cos[:, None, :], angle_sin[:, None, :])
        full_query = jnp.concatenate([shaped[..., :nope], turned], axis=-1)
        keys = jnp.dot(latent_normed, up_key, preferred_element_type=jnp.float32).astype(jnp.bfloat16)
        values = jnp.dot(latent_normed, up_value, preferred_element_type=jnp.float32).astype(jnp.bfloat16)
        return attend(full_query, keys.reshape(length, heads, nope), rotated_key, values.reshape(length, heads, width), nope)
    attn_small = group(query_small, up_key_small, up_value_small, HEADS_SMALL, NOPE_SMALL, VALUE_SMALL)
    attn_large = group(query_large, up_key_large, up_value_large, HEADS_LARGE, NOPE_LARGE, VALUE_LARGE)
    border = HEADS_SMALL * VALUE_SMALL
    mixed = jnp.dot(attn_small, out_weight[:border], preferred_element_type=jnp.float32)
    mixed = mixed + jnp.dot(attn_large, out_weight[border:], preferred_element_type=jnp.float32)
    middle = (resid.astype(jnp.float32) + mixed).astype(jnp.bfloat16)
    middle_wide = lax.optimization_barrier(middle).astype(jnp.float32)
    mixer_in = norm_rows(middle, mix_gain)
    gate = jnp.dot(mixer_in, gate_weight, preferred_element_type=jnp.float32)
    upward = jnp.dot(mixer_in, up_weight, preferred_element_type=jnp.float32)
    hidden = (jax.nn.silu(gate) * upward).astype(jnp.bfloat16)
    width = FF // N_TP
    total = middle_wide
    for index in range(N_TP):
        part = jnp.dot(hidden[:, index * width:(index + 1) * width], jnp.transpose(down_weight[:, index * width:(index + 1) * width]), preferred_element_type=jnp.float32).astype(jnp.bfloat16)
        total = total + lax.optimization_barrier(part).astype(jnp.float32)
    return total.astype(jnp.bfloat16)
```

```python
import functools
import math

import jax
import jax.numpy as jnp
from jax import lax
from jax.experimental import pallas as pl
from jax.experimental.pallas import tpu as pltpu
from jax.sharding import PartitionSpec as P

HEADS_SMALL = 8
NOPE_SMALL = 64
NOPE_LARGE = 128
VALUE_SMALL = 64
VALUE_LARGE = 128
ROTARY = 32


THETA = 10000.0
EPSILON = 1e-06
FLOOR = -1e30


def angles(positions, width):
    inverse = THETA ** (-jnp.arange(0, width, 2).astype(jnp.float32) / width)
    phase = positions.astype(jnp.float32)[:, None] * inverse[None, :]
    return (jnp.cos(phase), jnp.sin(phase))


def rotate(values, angle_cos, angle_sin):
    half = values.shape[-1] // 2
    first = values[..., :half].astype(jnp.float32)
    second = values[..., half:].astype(jnp.float32)
    turned = jnp.concatenate(
        [first * angle_cos - second * angle_sin, second * angle_cos + first * angle_sin], axis=-1
    )
    return turned.astype(jnp.bfloat16)


def norm_rows(values, gain):
    wide = values.astype(jnp.float32)
    scaled = wide * lax.rsqrt(jnp.mean(wide * wide, axis=-1, keepdims=True) + EPSILON)
    return (scaled * gain.astype(jnp.float32)).astype(jnp.bfloat16)


LOG2E = math.log2(math.e)
TILE = 256
PAD = 16


def ring_place(index, count):
    return jnp.where(index % 2 == 0, index // 2, count - 1 - index // 2)


def ring_index(place, count):
    place = (place + 2 * count) % count
    return jnp.where(place < count // 2, 2 * place, 2 * (count - 1 - place) + 1)


def attend_and_gather(count, shapes, *refs):
    (shared, expand_key, expand_value, query_small, query_large, gate, up) = refs[:7]
    out, gate_all, up_all = refs[7:10]
    maxima, sums, send_sem, recv_sem, own_sem = refs[10:]
    me = lax.axis_index("sp")
    place = ring_place(me, count)
    right, left = ring_index(place + 1, count), ring_index(place - 1, count)
    weights, wholes = (gate, up), (gate_all, up_all)
    depth = gate.shape[0]
    half = depth // 2
    last = count // 2

    barrier = pltpu.get_barrier_semaphore()
    for side in (right, left):
        pl.semaphore_signal(
            barrier, inc=1, device_id={"sp": side}, device_id_type=pl.DeviceIdType.MESH
        )
    pl.semaphore_wait(barrier, 2)

    def hop(way, step, which):
        origin = ring_index(place - (step - 1) if way == 0 else place + (step - 1), count)
        source = weights[which] if step == 1 else wholes[which].at[origin]
        target = wholes[which].at[origin]
        if step == last:
            span = pl.ds(way * half, half)
            source, target = source.at[span], target.at[span]
        return pltpu.make_async_remote_copy(
            src_ref=source,
            dst_ref=target,
            send_sem=send_sem.at[way, step - 1, which],
            recv_sem=recv_sem.at[way, step - 1, which],
            device_id={"sp": right if way == 0 else left},
            device_id_type=pl.DeviceIdType.MESH,
        )

    def own(which):
        return pltpu.make_async_copy(weights[which], wholes[which].at[me], own_sem.at[which])

    for which in range(2):
        for way in range(2):
            hop(way, 1, which).start()
    for which in range(2):
        own(which).start()

    events = [(step, which) for step in range(1, last) for which in range(2)]

    def forward(step, which):
        for way in range(2):
            hop(way, step, which).wait_recv()
            hop(way, step + 1, which).start()

    maxima[...] = jnp.full(maxima.shape, FLOOR, jnp.float32)
    sums[...] = jnp.zeros(sums.shape, jnp.float32)
    rows = query_small.shape[-1]

    def block(index, diagonal):
        start = pl.multiple_of(index * rows, rows)
        latent = shared[pl.ds(start, rows), :]
        for head, (group, inner, nope, wide, key_at, width, value_at, sum_at, out_at) in enumerate(shapes):
            key = jnp.dot(
                latent, expand_key[:, key_at : key_at + wide], preferred_element_type=jnp.float32
            ).astype(jnp.bfloat16)
            value = lax.dot_general(
                expand_value[value_at : value_at + width, :],
                latent,
                (((1,), (1,)), ((), ())),
                preferred_element_type=jnp.float32,
            ).astype(jnp.bfloat16)
            value = jnp.concatenate([value, jnp.ones((PAD, rows), jnp.bfloat16)], axis=0)
            scale = LOG2E / math.sqrt(nope + ROTARY)
            query = query_small if group == 0 else query_large
            for tile in range(rows // TILE):
                columns = slice(tile * TILE, (tile + 1) * TILE)
                length = (tile + 1) * TILE if diagonal else rows
                scores = jnp.dot(
                    key[:length], query[inner, :, columns], preferred_element_type=jnp.float32
                )
                if diagonal:
                    key_pos = lax.broadcasted_iota(jnp.int32, scores.shape, 0)
                    query_pos = lax.broadcasted_iota(jnp.int32, scores.shape, 1) + tile * TILE
                    scores = jnp.where(key_pos <= query_pos, scores, FLOOR)
                old = maxima[head, :, columns]
                new = jnp.maximum(old, jnp.max(scores, axis=0, keepdims=True))
                weight = jnp.exp2((scores - new) * scale).astype(jnp.bfloat16)
                factor = jnp.exp2((old - new) * scale)
                place_of = slice(sum_at, sum_at + width + PAD)
                total = sums[place_of, columns] * factor + jnp.dot(
                    value[:, :length], weight, preferred_element_type=jnp.float32
                )
                if diagonal:
                    out[out_at : out_at + width, columns] = (
                        total[:width] / total[width : width + 1]
                    ).astype(jnp.bfloat16)
                else:
                    maxima[head, :, columns] = new
                    sums[place_of, columns] = total

    def step_of(index, carry):
        for number, event in enumerate(events):

            @pl.when(index == 2 * number + 2)
            def _():
                forward(*event)

        block(index, False)
        return carry

    lax.fori_loop(0, me, step_of, 0)
    block(me, True)
    for number, event in enumerate(events):

        @pl.when(me <= 2 * number + 2)
        def _():
            forward(*event)

    for which in range(2):
        own(which).wait()
        for way in range(2):
            hop(way, last, which).wait_recv()
            for step in range(1, last + 1):
                hop(way, step, which).wait_send()


def on_device(
    count,
    resid,
    query_small,
    query_large,
    kv_latent,
    rope_key,
    kv_gain,
    up_key_small,
    up_value_small,
    up_key_large,
    up_value_large,
    out_weight,
    mix_gain,
    gate_weight,
    up_weight,
    down_weight,
):
    rows, latent_size = kv_latent.shape
    offset = lax.axis_index("sp") * rows
    positions = offset + jnp.arange(rows, dtype=jnp.int32)
    angle_cos, angle_sin = angles(positions, ROTARY)
    shared = jnp.concatenate(
        [norm_rows(kv_latent, kv_gain), rotate(rope_key, angle_cos, angle_sin)], axis=1
    )
    shared = jnp.pad(lax.all_gather(shared, "sp", axis=0, tiled=True), ((0, 0), (0, 128 - ROTARY)))
    resid, down_weight, shared = lax.optimization_barrier((resid, down_weight, shared))
    resid_all = lax.all_gather(resid, "tp", axis=0, tiled=True)
    down_whole = lax.all_gather(down_weight, "sp", axis=0, tiled=True)

    shapes = []
    queries, keys, values = [], [], []
    key_at = value_at = sum_at = 0
    for group, (query, up_key, up_value, nope, width) in enumerate(
        (
            (query_small, up_key_small, up_value_small, NOPE_SMALL, VALUE_SMALL),
            (query_large, up_key_large, up_value_large, NOPE_LARGE, VALUE_LARGE),
        )
    ):
        heads = up_key.shape[1] // nope
        wide = nope + ROTARY
        padded = -(-wide // 128) * 128
        shaped = query.reshape(rows, heads, wide)
        turned = rotate(shaped[..., nope:], angle_cos[:, None, :], angle_sin[:, None, :])
        full = jnp.concatenate([shaped[..., :nope], turned], axis=-1)
        full = jnp.pad(full, ((0, 0), (0, 0), (0, padded - wide)))
        queries.append(jnp.transpose(full, (1, 2, 0)))
        rotary_part = jnp.eye(128, padded, k=nope, dtype=jnp.bfloat16)
        rotary_part = jnp.where(jnp.arange(128)[:, None] < ROTARY, rotary_part, 0)
        for head in range(heads):
            part = jnp.pad(up_key[:, head * nope : (head + 1) * nope], ((0, 0), (0, padded - nope)))
            keys.append(jnp.concatenate([part, rotary_part.astype(jnp.bfloat16)], axis=0))
            shapes.append((group, head, nope, padded, key_at, width, value_at, sum_at, value_at))
            key_at += padded
            value_at += width
            sum_at += width + PAD
        values.append(jnp.pad(jnp.transpose(up_value), ((0, 0), (0, 128))))
    expand_key = jnp.concatenate(keys, axis=1)
    expand_value = jnp.concatenate(values, axis=0)
    depth, hidden_size = gate_weight.shape
    vmem = pl.BlockSpec(memory_space=pltpu.VMEM)
    hbm = pl.BlockSpec(memory_space=pl.ANY)
    whole = jax.ShapeDtypeStruct((count, depth, hidden_size), jnp.bfloat16)
    attn, gate_whole, up_whole = pl.pallas_call(
        functools.partial(attend_and_gather, count, tuple(shapes)),
        out_shape=(jax.ShapeDtypeStruct((value_at, rows), jnp.bfloat16), whole, whole),
        in_specs=[vmem] * 5 + [hbm] * 2,
        out_specs=(vmem, hbm, hbm),
        scratch_shapes=[
            pltpu.VMEM((len(shapes), 1, rows), jnp.float32),
            pltpu.VMEM((sum_at, rows), jnp.float32),
            pltpu.SemaphoreType.DMA((2, count // 2, 2)),
            pltpu.SemaphoreType.DMA((2, count // 2, 2)),
            pltpu.SemaphoreType.DMA((2,)),
        ],
        compiler_params=pltpu.CompilerParams(
            collective_id=0, has_side_effects=True, vmem_limit_bytes=50 * 2**20
        ),
        cost_estimate=pl.CostEstimate(
            flops=10**11, bytes_accessed=3 * 10**7, transcendentals=2 * 10**7
        ),
    )(shared, expand_key, expand_value, queries[0], queries[1], gate_weight, up_weight)
    gate_whole = gate_whole.reshape(count * depth, hidden_size)
    up_whole = up_whole.reshape(count * depth, hidden_size)
    border_device = up_value_small.shape[1]
    attn_all = lax.all_gather(attn, "tp", axis=0)
    attn_small = attn_all[:, :border_device].reshape(-1, rows)
    attn_large = attn_all[:, border_device:].reshape(-1, rows)
    border = HEADS_SMALL * VALUE_SMALL
    over_first = (((0,), (0,)), ((), ()))
    mixed = lax.dot_general(
        attn_small, out_weight[:border], over_first, preferred_element_type=jnp.float32
    )
    mixed = mixed + lax.dot_general(
        attn_large, out_weight[border:], over_first, preferred_element_type=jnp.float32
    )
    middle_all = (resid_all.astype(jnp.float32) + mixed).astype(jnp.bfloat16)
    mixer_in = norm_rows(middle_all, mix_gain)
    gate = jnp.dot(mixer_in, gate_whole, preferred_element_type=jnp.float32)
    upward = jnp.dot(mixer_in, up_whole, preferred_element_type=jnp.float32)
    hidden = (jax.nn.silu(gate) * upward).astype(jnp.bfloat16)
    branch = lax.psum_scatter(
        lax.dot_general(
            hidden, down_whole, (((1,), (1,)), ((), ())), preferred_element_type=jnp.float32
        ).astype(jnp.bfloat16),
        "tp",
        scatter_dimension=0,
        tiled=True,
    ).astype(jnp.float32)
    middle = lax.dynamic_slice_in_dim(
        middle_all, lax.axis_index("tp") * resid.shape[0], resid.shape[0], 0
    )
    return (middle.astype(jnp.float32) + branch).astype(jnp.bfloat16)


def solution(mesh):
    placed = (
        P(("sp", "tp"), None),
        P("sp", "tp"),
        P("sp", "tp"),
        P("sp", None),
        P("sp", None),
        P(),
        P(None, "tp"),
        P(None, "tp"),
        P(None, "tp"),
        P(None, "tp"),
        P(),
        P(),
        P("sp", "tp"),
        P("sp", "tp"),
        P("sp", "tp"),
    )
    return jax.shard_map(
        functools.partial(on_device, mesh.shape["sp"]), mesh=mesh, in_specs=placed, out_specs=P(("sp", "tp"), None), check_vma=False
    )
```

```python
import functools
import math

import jax
import jax.numpy as jnp
from jax import lax
from jax.experimental import pallas as pl
from jax.experimental.pallas import tpu as pltpu
from jax.sharding import PartitionSpec as P

HEADS_SMALL = 8
NOPE_SMALL = 64
NOPE_LARGE = 128
VALUE_SMALL = 64
VALUE_LARGE = 128
ROTARY = 32


THETA = 10000.0
EPSILON = 1e-06
FLOOR = -1e30


def angles(positions, width):
    inverse = THETA ** (-jnp.arange(0, width, 2).astype(jnp.float32) / width)
    phase = positions.astype(jnp.float32)[:, None] * inverse[None, :]
    return (jnp.cos(phase), jnp.sin(phase))


def rotate(values, angle_cos, angle_sin):
    half = values.shape[-1] // 2
    first = values[..., :half].astype(jnp.float32)
    second = values[..., half:].astype(jnp.float32)
    turned = jnp.concatenate(
        [first * angle_cos - second * angle_sin, second * angle_cos + first * angle_sin], axis=-1
    )
    return turned.astype(jnp.bfloat16)


def norm_rows(values, gain):
    wide = values.astype(jnp.float32)
    scaled = wide * lax.rsqrt(jnp.mean(wide * wide, axis=-1, keepdims=True) + EPSILON)
    return (scaled * gain.astype(jnp.float32)).astype(jnp.bfloat16)


LOG2E = math.log2(math.e)
TILE = 256
PAD = 16


def ring_place(index, count):
    return jnp.where(index % 2 == 0, index // 2, count - 1 - index // 2)


def ring_index(place, count):
    place = (place + 2 * count) % count
    return jnp.where(place < count // 2, 2 * place, 2 * (count - 1 - place) + 1)


def attend_and_gather(count, owners, shapes, *refs):
    (shared, expand_key, expand_value, query_small, query_large, resid, gate, up, down) = refs[:9]
    attn_all, resid_all, gate_all, up_all, down_all = refs[9:14]
    out, maxima, sums, send_sem, recv_sem, own_sem, peer_send, peer_recv = refs[14:]
    column = lax.axis_index("tp")
    me = lax.axis_index("sp")
    place = ring_place(me, count)
    right, left = ring_index(place + 1, count), ring_index(place - 1, count)
    weights, wholes = (gate, up, down), (gate_all, up_all, down_all)
    parts = len(weights)
    depth = gate.shape[0]
    half = depth // 2
    last = count // 2

    barrier = pltpu.get_barrier_semaphore()
    for side in (right, left):
        pl.semaphore_signal(
            barrier, inc=1, device_id={"sp": side}, device_id_type=pl.DeviceIdType.MESH
        )
    for ahead in range(1, owners):
        pl.semaphore_signal(
            barrier,
            inc=1,
            device_id={"tp": lax.rem(column + ahead, owners)},
            device_id_type=pl.DeviceIdType.MESH,
        )
    pl.semaphore_wait(barrier, 1 + owners)

    def share(source, whole, ahead, which):
        return pltpu.make_async_remote_copy(
            src_ref=source,
            dst_ref=whole.at[column],
            send_sem=peer_send.at[which, ahead],
            recv_sem=peer_recv.at[which, ahead],
            device_id={"tp": lax.rem(column + ahead, owners)},
            device_id_type=pl.DeviceIdType.MESH,
        )

    def hop(way, step, which):
        origin = ring_index(place - (step - 1) if way == 0 else place + (step - 1), count)
        source = weights[which] if step == 1 else wholes[which].at[origin]
        target = wholes[which].at[origin]
        if step == last:
            span = pl.ds(way * half, half)
            source, target = source.at[span], target.at[span]
        return pltpu.make_async_remote_copy(
            src_ref=source,
            dst_ref=target,
            send_sem=send_sem.at[way, step - 1, which],
            recv_sem=recv_sem.at[way, step - 1, which],
            device_id={"sp": right if way == 0 else left},
            device_id_type=pl.DeviceIdType.MESH,
        )

    def own(which):
        return pltpu.make_async_copy(weights[which], wholes[which].at[me], own_sem.at[which])

    keep_resid = pltpu.make_async_copy(resid, resid_all.at[column], own_sem.at[parts])
    keep_attn = pltpu.make_async_copy(out, attn_all.at[column], own_sem.at[parts + 1])

    for which in range(parts):
        for way in range(2):
            hop(way, 1, which).start()
    for ahead in range(1, owners):
        share(resid, resid_all, ahead, 0).start()
    for which in range(parts):
        own(which).start()
    keep_resid.start()

    events = [(step, which) for step in range(1, last) for which in range(parts)]

    def forward(step, which):
        for way in range(2):
            hop(way, step, which).wait_recv()
            hop(way, step + 1, which).start()

    maxima[...] = jnp.full(maxima.shape, FLOOR, jnp.float32)
    sums[...] = jnp.zeros(sums.shape, jnp.float32)
    rows = query_small.shape[-1]

    def block(index, diagonal):
        start = pl.multiple_of(index * rows, rows)
        latent = shared[pl.ds(start, rows), :]
        for head, (group, inner, nope, wide, key_at, width, value_at, sum_at, out_at) in enumerate(shapes):
            key = jnp.dot(
                latent, expand_key[:, key_at : key_at + wide], preferred_element_type=jnp.float32
            ).astype(jnp.bfloat16)
            value = lax.dot_general(
                expand_value[value_at : value_at + width, :],
                latent[:, : expand_value.shape[1]],
                (((1,), (1,)), ((), ())),
                preferred_element_type=jnp.float32,
            ).astype(jnp.bfloat16)
            value = jnp.concatenate([value, jnp.ones((PAD, rows), jnp.bfloat16)], axis=0)
            scale = LOG2E / math.sqrt(nope + ROTARY)
            query = query_small if group == 0 else query_large
            for tile in range(rows // TILE):
                columns = slice(tile * TILE, (tile + 1) * TILE)
                length = (tile + 1) * TILE if diagonal else rows
                scores = jnp.dot(
                    key[:length], query[inner, :, columns], preferred_element_type=jnp.float32
                )
                if diagonal:
                    key_pos = lax.broadcasted_iota(jnp.int32, scores.shape, 0)
                    query_pos = lax.broadcasted_iota(jnp.int32, scores.shape, 1) + tile * TILE
                    scores = jnp.where(key_pos <= query_pos, scores, FLOOR)
                old = maxima[head, :, columns]
                new = jnp.maximum(old, jnp.max(scores, axis=0, keepdims=True))
                weight = jnp.exp2((scores - new) * scale).astype(jnp.bfloat16)
                factor = jnp.exp2((old - new) * scale)
                place_of = slice(sum_at, sum_at + width + PAD)
                total = sums[place_of, columns] * factor + jnp.dot(
                    value[:, :length], weight, preferred_element_type=jnp.float32
                )
                if diagonal:
                    out[out_at : out_at + width, columns] = (
                        total[:width] / total[width : width + 1]
                    ).astype(jnp.bfloat16)
                else:
                    maxima[head, :, columns] = new
                    sums[place_of, columns] = total

    def step_of(index, carry):
        for number, event in enumerate(events):

            @pl.when(index == 2 * number + 2)
            def _():
                forward(*event)

        block(index, False)
        return carry

    lax.fori_loop(0, me, step_of, 0)
    block(me, True)
    for ahead in range(1, owners):
        share(out, attn_all, ahead, 1).start()
    keep_attn.start()
    for number, event in enumerate(events):

        @pl.when(me <= 2 * number + 2)
        def _():
            forward(*event)

    keep_resid.wait()
    keep_attn.wait()
    for ahead in range(1, owners):
        share(resid, resid_all, ahead, 0).wait()
        share(out, attn_all, ahead, 1).wait()
    for which in range(parts):
        own(which).wait()
        for way in range(2):
            hop(way, last, which).wait_recv()
            for step in range(1, last + 1):
                hop(way, step, which).wait_send()


def on_device(
    count,
    owners,
    resid,
    query_small,
    query_large,
    kv_latent,
    rope_key,
    kv_gain,
    up_key_small,
    up_value_small,
    up_key_large,
    up_value_large,
    out_weight,
    mix_gain,
    gate_weight,
    up_weight,
    down_weight,
):
    rows, latent_size = kv_latent.shape
    offset = lax.axis_index("sp") * rows
    positions = offset + jnp.arange(rows, dtype=jnp.int32)
    angle_cos, angle_sin = angles(positions, ROTARY)
    shared = jnp.concatenate(
        [norm_rows(kv_latent, kv_gain), rotate(rope_key, angle_cos, angle_sin)], axis=1
    )
    shared = lax.all_gather(shared, "sp", axis=0, tiled=True)

    shapes = []
    queries, keys, values = [], [], []
    key_at = value_at = sum_at = 0
    for group, (query, up_key, up_value, nope, width) in enumerate(
        (
            (query_small, up_key_small, up_value_small, NOPE_SMALL, VALUE_SMALL),
            (query_large, up_key_large, up_value_large, NOPE_LARGE, VALUE_LARGE),
        )
    ):
        heads = up_key.shape[1] // nope
        wide = nope + ROTARY
        padded = -(-wide // 128) * 128
        shaped = query.reshape(rows, heads, wide)
        turned = rotate(shaped[..., nope:], angle_cos[:, None, :], angle_sin[:, None, :])
        full = jnp.concatenate([shaped[..., :nope], turned], axis=-1)
        full = jnp.pad(full, ((0, 0), (0, 0), (0, padded - wide)))
        queries.append(jnp.transpose(full, (1, 2, 0)))
        rotary_part = jnp.eye(ROTARY, padded, k=nope, dtype=jnp.bfloat16)
        for head in range(heads):
            part = jnp.pad(up_key[:, head * nope : (head + 1) * nope], ((0, 0), (0, padded - nope)))
            keys.append(jnp.concatenate([part, rotary_part], axis=0))
            shapes.append((group, head, nope, padded, key_at, width, value_at, sum_at, value_at))
            key_at += padded
            value_at += width
            sum_at += width + PAD
        values.append(jnp.transpose(up_value))
    expand_key = jnp.concatenate(keys, axis=1)
    expand_value = jnp.concatenate(values, axis=0)
    depth, hidden_size = gate_weight.shape
    vmem = pl.BlockSpec(memory_space=pltpu.VMEM)
    hbm = pl.BlockSpec(memory_space=pl.ANY)
    whole = jax.ShapeDtypeStruct((count, depth, hidden_size), jnp.bfloat16)
    attn_all, resid_all, gate_whole, up_whole, down_whole = pl.pallas_call(
        functools.partial(attend_and_gather, count, owners, tuple(shapes)),
        out_shape=(
            jax.ShapeDtypeStruct((owners, value_at, rows), jnp.bfloat16),
            jax.ShapeDtypeStruct((owners,) + resid.shape, jnp.bfloat16),
            whole,
            whole,
            whole,
        ),
        in_specs=[vmem] * 5 + [hbm] * 4,
        out_specs=(hbm,) * 5,
        scratch_shapes=[
            pltpu.VMEM((value_at, rows), jnp.bfloat16),
            pltpu.VMEM((len(shapes), 1, rows), jnp.float32),
            pltpu.VMEM((sum_at, rows), jnp.float32),
            pltpu.SemaphoreType.DMA((2, count // 2, 3)),
            pltpu.SemaphoreType.DMA((2, count // 2, 3)),
            pltpu.SemaphoreType.DMA((5,)),
            pltpu.SemaphoreType.DMA((2, owners)),
            pltpu.SemaphoreType.DMA((2, owners)),
        ],
        compiler_params=pltpu.CompilerParams(
            collective_id=0, has_side_effects=True, vmem_limit_bytes=50 * 2**20
        ),
        cost_estimate=pl.CostEstimate(
            flops=10**11, bytes_accessed=3 * 10**7, transcendentals=2 * 10**7
        ),
    )(
        shared,
        expand_key,
        expand_value,
        queries[0],
        queries[1],
        resid,
        gate_weight,
        up_weight,
        down_weight,
    )
    resid_all = resid_all.reshape(rows, resid.shape[1])
    down_whole = down_whole.reshape(count * depth, hidden_size)
    gate_whole = gate_whole.reshape(count * depth, hidden_size)
    up_whole = up_whole.reshape(count * depth, hidden_size)
    border_device = up_value_small.shape[1]
    attn_small = attn_all[:, :border_device].reshape(-1, rows)
    attn_large = attn_all[:, border_device:].reshape(-1, rows)
    border = HEADS_SMALL * VALUE_SMALL
    over_first = (((0,), (0,)), ((), ()))
    mixed = lax.dot_general(
        attn_small, out_weight[:border], over_first, preferred_element_type=jnp.float32
    )
    mixed = mixed + lax.dot_general(
        attn_large, out_weight[border:], over_first, preferred_element_type=jnp.float32
    )
    middle_all = (resid_all.astype(jnp.float32) + mixed).astype(jnp.bfloat16)
    mixer_in = norm_rows(middle_all, mix_gain)
    gate = jnp.dot(mixer_in, gate_whole, preferred_element_type=jnp.float32)
    upward = jnp.dot(mixer_in, up_whole, preferred_element_type=jnp.float32)
    hidden = (jax.nn.silu(gate) * upward).astype(jnp.bfloat16)
    branch = lax.psum_scatter(
        lax.dot_general(
            hidden, down_whole, (((1,), (1,)), ((), ())), preferred_element_type=jnp.float32
        ).astype(jnp.bfloat16),
        "tp",
        scatter_dimension=0,
        tiled=True,
    ).astype(jnp.float32)
    middle = lax.dynamic_slice_in_dim(
        middle_all, lax.axis_index("tp") * resid.shape[0], resid.shape[0], 0
    )
    return (middle.astype(jnp.float32) + branch).astype(jnp.bfloat16)


def solution(mesh):
    placed = (
        P(("sp", "tp"), None),
        P("sp", "tp"),
        P("sp", "tp"),
        P("sp", None),
        P("sp", None),
        P(),
        P(None, "tp"),
        P(None, "tp"),
        P(None, "tp"),
        P(None, "tp"),
        P(),
        P(),
        P("sp", "tp"),
        P("sp", "tp"),
        P("sp", "tp"),
    )
    return jax.shard_map(
        functools.partial(on_device, mesh.shape["sp"], mesh.shape["tp"]), mesh=mesh, in_specs=placed, out_specs=P(("sp", "tp"), None), check_vma=False
    )
```
